32 devices in a mesh: rep: 2 (over y), fs: 4 (over z), tp: 4 (over x, core).
Axes of the slice: x: 2, y: 2, z: 4, core: 2. Of those that a mesh axis runs over, the one named last changes fastest.
Arguments:
- tokens: bfloat16 [8, 192, 2048], P(('rep', 'fs'), None, 'tp'), may hold values from -40 to 40
- ff_first: bfloat16 [2048, 2048], P('fs', 'tp'), may hold values from -0.125 to 0.125
- ff_second: bfloat16 [2048, 2048], P('fs', 'tp'), may hold values from -0.125 to 0.125
- ff_down: bfloat16 [2048, 2048], P('fs', 'tp'), may hold values from -0.125 to 0.125
- mix_stream: bfloat16 [2048, 2048], P('fs', 'tp'), may hold values from -0.125 to 0.125
- mix_gate: bfloat16 [2048, 2048], P('fs', 'tp'), may hold values from -0.125 to 0.125
- mix_down: bfloat16 [2048, 2048], P('fs', 'tp'), may hold values from -0.125 to 0.125
- gain_one: float32 [2048], P('tp'), may hold values from 0.1 to 1.9
- gain_two: float32 [2048], P('tp'), may hold values from 0.1 to 1.9
- gain_three: float32 [2048], P('tp'), may hold values from 0.1 to 1.9
Outputs:
- layer_out: bfloat16 [8, 192, 2048], P(('rep', 'fs'), None, 'tp')
The draws below stay inside these ranges and needn't reach their ends.
All inputs are finite; a program needn't handle non-finite values.
Results may differ from the reference program's by a relative error of at most 0.01.
Values may be sent and summed in bfloat16 or wider, within the bound.
A program may use at most 64 MiB of HBM per device.

```python
import jax
import jax.numpy as jnp
from jax import lax

D = 2048
FF = 2048
SEQ = 192
BATCH = 8


def draw_tokens(key, part):
    normal_draw = jax.random.truncated_normal(key, -5.0, 5.0, (BATCH, SEQ, D), jnp.float32)
    column_ramp = jnp.arange(D, dtype=jnp.float32) / D
    values = normal_draw * 0.6 * 3.0 ** column_ramp[None, None, :]
    return values.astype(jnp.bfloat16)


def level_of(own_key, shape, cuts, smallest, largest):
    def one(axis_at, blocks):
        draws = jax.random.uniform(jax.random.fold_in(jax.random.fold_in(own_key, 6), axis_at), (blocks,), jnp.float32, smallest / len(cuts), largest / len(cuts))
        return jnp.repeat(jnp.exp(draws), shape[axis_at] // blocks).reshape((-1,) + (1,) * (len(shape) - axis_at - 1))

    level = one(*cuts[0])
    for cut in cuts[1:]:
        level = level * one(*cut)
    return level


def bell_draw(key, extent, deviation, bound, cuts=(), kind=jnp.bfloat16):
    array = jax.random.normal(key, extent, jnp.float32) * deviation
    if len(cuts) > 0:
        array = level_of(key, extent, cuts, -0.22, 0.18) * array
    return jnp.clip(array, min=-bound, max=bound).astype(kind)


def setup_inputs(seed: int = 0) -> dict:
    splits = jax.random.split(jax.random.key(seed), 11)
    tokens = draw_tokens(jax.random.fold_in(splits[10], 71), 0)
    ff_first = bell_draw(splits[1], (D, FF), D ** -0.5, 0.125, ((0, 4), (1, 4)))
    ff_second = bell_draw(splits[2], (D, FF), D ** -0.5, 0.125, ((0, 4), (1, 4)))
    ff_down = bell_draw(splits[3], (FF, D), FF ** -0.5, 0.125, ((0, 4), (1, 4)))
    mix_stream = bell_draw(splits[4], (D, D), D ** -0.5, 0.125, ((0, 4), (1, 4)))
    mix_gate = bell_draw(splits[5], (D, D), D ** -0.5, 0.125, ((0, 4), (1, 4)))
    mix_down = bell_draw(splits[6], (D, D), D ** -0.5, 0.125, ((0, 4), (1, 4)))
    gain_one = jnp.clip(1.0 + 0.18 * jax.random.normal(splits[7], (D,), jnp.float32), 0.1, 1.9)
    gain_two = jnp.clip(1.0 + 0.18 * jax.random.normal(splits[8], (D,), jnp.float32), 0.1, 1.9)
    gain_three = jnp.clip(1.0 + 0.18 * jax.random.normal(splits[9], (D,), jnp.float32), 0.1, 1.9)
    return dict(tokens=tokens, ff_first=ff_first, ff_second=ff_second, ff_down=ff_down, mix_stream=mix_stream, mix_gate=mix_gate, mix_down=mix_down, gain_one=gain_one, gain_two=gain_two, gain_three=gain_three)


alpha_scale = 2.0 ** 0.5
norm_eps = 1e-05

def matmul(inputs, weight):
    flat_rows = inputs.reshape(-1, inputs.shape[-1])
    result = jnp.dot(flat_rows, weight, preferred_element_type=jnp.float32)
    return result.reshape(inputs.shape[:-1] + (weight.shape[1],))

def layer_norm(summed, gain_vec):
    row_mean = lax.optimization_barrier(jnp.mean(summed, axis=-1, keepdims=True))
    row_var = lax.optimization_barrier(jnp.mean(jnp.square(summed - row_mean), axis=-1, keepdims=True))
    normed = (summed - row_mean) * lax.rsqrt(row_var + norm_eps)
    return (normed * gain_vec.astype(jnp.float32)).astype(jnp.bfloat16)

def half_step(inputs, first_w, second_w, down_w, gain_vec):
    hidden = (jax.nn.silu(matmul(inputs, first_w)) * matmul(inputs, second_w)).astype(jnp.bfloat16)
    return layer_norm(alpha_scale * inputs.astype(jnp.float32) + 0.5 * matmul(hidden, down_w), gain_vec)

def pool_mix(inputs, stream_w, gate_w, down_w, gain_vec):
    stream = matmul(inputs, stream_w).astype(jnp.bfloat16)
    gate_act = matmul(inputs, gate_w)
    length = stream.shape[1]
    width = stream.shape[2]
    running = jnp.cumsum(stream.astype(jnp.float32), axis=1)
    positions = jnp.arange(length)
    channel_group = jnp.arange(width) * 4 // width
    pooled = jnp.zeros_like(running)
    for scale_level in range(4):
        window = 2 << scale_level
        lagged = jnp.pad(running, ((0, 0), (window, 0), (0, 0)))[:, :length]
        counts = jnp.minimum(positions + 1, window).astype(jnp.float32)
        window_mean = (running - lagged) / counts[None, :, None]
        pooled = jnp.where((channel_group == scale_level)[None, None, :], window_mean, pooled)
    pooled = pooled - stream.astype(jnp.float32)
    mixed_rows = (pooled * jax.nn.silu(gate_act)).astype(jnp.bfloat16)
    return layer_norm(alpha_scale * inputs.astype(jnp.float32) + matmul(mixed_rows, down_w), gain_vec)

def reference(tokens, ff_first, ff_second, ff_down, mix_stream, mix_gate, mix_down, gain_one, gain_two, gain_three):
    first = half_step(tokens, ff_first, ff_second, ff_down, gain_one)
    second = pool_mix(first, mix_stream, mix_gate, mix_down, gain_two)
    return half_step(second, ff_first, ff_second, ff_down, gain_three)
```

```python
import functools

import jax
import jax.numpy as jnp
from jax import lax
from jax.experimental import pallas as pl
from jax.experimental.pallas import tpu as pltpu
from jax.sharding import PartitionSpec as P

alpha_scale = 2.0**0.5
norm_eps = 1e-05


def product(inputs, weight):
    return jnp.einsum("bsd,df->bsf", inputs, weight, preferred_element_type=jnp.float32)


def widen(local_rows):
    return lax.all_gather(local_rows, "tp", axis=2, tiled=True)


def norm_cols(summed, gain_vec):
    width = summed.shape[-1] * lax.axis_size("tp")
    totals, squares = lax.psum((jnp.sum(summed, axis=-1), jnp.sum(summed * summed, axis=-1)), "tp")
    row_mean = totals / width
    row_var = squares / width - row_mean * row_mean
    normed = (summed - row_mean[..., None]) * lax.rsqrt(row_var[..., None] + norm_eps)
    return (normed * gain_vec[None, None, :]).astype(jnp.bfloat16)


def half_step(local_rows, project_in, project_out, gain_vec):
    whole = widen(local_rows)
    first_act, second_act = project_in(whole)
    hidden = (jax.nn.silu(first_act) * second_act).astype(jnp.bfloat16)
    wide_hidden = lax.all_gather(hidden, "tp", axis=2, tiled=True)
    branch = project_out(wide_hidden)
    return norm_cols(alpha_scale * local_rows.astype(jnp.float32) + 0.5 * branch, gain_vec)


def pool_mix(local_rows, project_in, project_out, gain_vec):
    whole = widen(local_rows)
    stream_act, gate_act = project_in(whole)
    stream = stream_act.astype(jnp.bfloat16)
    length = stream.shape[1]
    channel_group = lax.axis_index("tp") * 4 // lax.axis_size("tp")
    window = lax.shift_left(jnp.int32(2), channel_group)
    later = lax.broadcasted_iota(jnp.int32, (length, length), 0)
    earlier = lax.broadcasted_iota(jnp.int32, (length, length), 1)
    offset = later - earlier
    band = ((offset >= 0) & (offset < window)).astype(jnp.bfloat16)
    window_sums = jnp.einsum("ts,bsc->btc", band, stream, preferred_element_type=jnp.float32)
    counts = jnp.minimum(jnp.arange(length, dtype=jnp.int32) + 1, window).astype(jnp.float32)
    pooled = window_sums / counts[None, :, None] - stream.astype(jnp.float32)
    gated = (pooled * jax.nn.silu(gate_act)).astype(jnp.bfloat16)
    wide_gated = lax.all_gather(gated, "tp", axis=2, tiled=True)
    branch = project_out(wide_gated)
    return norm_cols(alpha_scale * local_rows.astype(jnp.float32) + branch, gain_vec)


def shards(
    tokens,
    ff_first,
    ff_second,
    ff_down,
    mix_stream,
    mix_gate,
    mix_down,
    gain_one,
    gain_two,
    gain_three,
):
    collected = (
        lax.all_gather(ff_first, "fs", axis=0, tiled=True),
        lax.all_gather(ff_second, "fs", axis=0, tiled=True),
        lax.all_gather(ff_down, "fs", axis=0, tiled=True),
        lax.all_gather(mix_stream, "fs", axis=0, tiled=True),
        lax.all_gather(mix_gate, "fs", axis=0, tiled=True),
        lax.all_gather(mix_down, "fs", axis=0, tiled=True),
    )

    def ffn_in(whole):
        return (product(whole, collected[0]), product(whole, collected[1]))

    def ffn_out(wide_rows):
        return product(wide_rows, collected[2])

    def mix_in(whole):
        return (product(whole, collected[3]), product(whole, collected[4]))

    def mix_out(wide_rows):
        return product(wide_rows, collected[5])

    first = half_step(tokens, ffn_in, ffn_out, gain_one)
    second = pool_mix(first, mix_in, mix_out, gain_two)
    return half_step(second, ffn_in, ffn_out, gain_three)


N_WEIGHTS = 6
MESH = pl.DeviceIdType.MESH


def hub_kernel(
    axis_sizes,
    tok,
    wa,
    wb,
    wc,
    ws,
    wg,
    wm,
    gain_one,
    gain_two,
    gain_three,
    out,
    wbuf,
    acts,
    stat,
    landed,
    tok_sem,
    end_send,
    end_recv,
    mid_send,
    mid_recv,
    rep_send,
    rep_recv,
    tp_send,
    tp_recv,
    stat_send,
    stat_recv,
    out_sem,
):
    n_fs, n_tp = axis_sizes
    weights = (wa, wb, wc, ws, wg, wm)
    rows, width = tok.shape
    depth = wa.shape[0]
    half = depth // 2
    features = width * n_tp
    r = lax.axis_index("rep")
    z = lax.axis_index("fs")
    j = lax.axis_index("tp")
    side = r % 2
    pair = r + 1 - 2 * side
    core_peer = j + 1 - 2 * (j % 2)
    chip_peer = (j + 2) % n_tp
    cross_peer = (core_peer + 2) % n_tp
    upper = z // 2
    is_hub = (z + 1) // 2 == 1
    my_end = upper * (n_fs - 1)
    my_hub = 1 + upper
    other_hub = n_fs - 1 - my_hub
    other_end = n_fs - 1 - my_end

    barrier = pltpu.get_barrier_semaphore()

    def greet(**where):
        pl.semaphore_signal(barrier, inc=1, device_id=where, device_id_type=MESH)

    greet(tp=core_peer)
    greet(tp=chip_peer)
    greet(tp=cross_peer)

    @pl.when(is_hub)
    def _():
        greet(rep=pair)
        greet(fs=other_hub)
        greet(fs=my_end)
        pl.semaphore_wait(barrier, 6)

    @pl.when(jnp.logical_not(is_hub))
    def _():
        greet(fs=my_hub)
        pl.semaphore_wait(barrier, 4)

    def remote(src, dst, send_sem, recv_sem, **where):
        return pltpu.make_async_remote_copy(
            src_ref=src, dst_ref=dst, send_sem=send_sem, recv_sem=recv_sem, device_id=where, device_id_type=MESH
        )

    def part(ref, which):
        return ref.at[pl.ds(pl.multiple_of(which * half, half), half)]

    def seq(ref, s):
        return ref.at[pl.ds(s * rows, rows)]

    def tok_copy():
        return remote(tok, seq(acts.at[0, j], 1), tok_sem.at[0], tok_sem.at[1], fs=my_hub)

    def end_copy(w, order):
        which = side if order == 0 else 1 - side
        return remote(part(weights[w], which), part(wbuf.at[w, 0], which), end_send.at[w, order], end_recv.at[w, order], fs=my_hub)

    @pl.when(jnp.logical_not(is_hub))
    def _():
        started = [tok_copy()] + [end_copy(w, order) for w in range(N_WEIGHTS) for order in range(2)]
        for copy in started:
            copy.start()
        for copy in started:
            copy.wait_send()
        remote(landed, landed, out_sem.at[0], out_sem.at[1], fs=my_hub).wait_recv()
        out[...] = landed[...]

    @pl.when(is_hub)
    def _():
        started = []

        def go(copy):
            copy.start()
            started.append(copy)

        def own_out(w):
            go(remote(part(weights[w], side), part(wbuf.at[w, 1], side), mid_send.at[w, 0], mid_recv.at[w, 0], fs=other_hub))

        def end_through(w):
            end_copy(w, 0).wait_recv()
            go(remote(part(wbuf.at[w, 0], side), part(wbuf.at[w, 2], side), mid_send.at[w, 1], mid_recv.at[w, 1], fs=other_hub))

        def share(w, slot):
            piece = part(wbuf.at[w, 1 + slot], side)
            remote(piece, piece, mid_send.at[w, slot], mid_recv.at[w, slot], fs=other_hub).wait_recv()
            go(remote(piece, piece, rep_send.at[w, slot], rep_recv.at[w, slot], rep=pair))

        def complete(w):
            end_copy(w, 1).wait_recv()
            for slot in range(2):
                piece = part(wbuf.at[w, 1 + slot], 1 - side)
                remote(piece, piece, rep_send.at[w, slot], rep_recv.at[w, slot], rep=pair).wait_recv()

        def block_of(k, owner, s):
            return seq(acts.at[k, owner], s)

        def spread(k, s, src=None):
            mine = block_of(k, j, s)
            src = mine if src is None else src
            go(remote(src, mine, tp_send.at[k, s, 1], tp_recv.at[k, s, 1], tp=chip_peer))
            go(remote(src, mine, tp_send.at[k, s, 0], tp_recv.at[k, s, 0], tp=core_peer))

        def relay(k, s):
            there = block_of(k, chip_peer, s)
            remote(there, there, tp_send.at[k, s, 1], tp_recv.at[k, s, 1], tp=chip_peer).wait_recv()
            go(remote(there, there, tp_send.at[k, s, 2], tp_recv.at[k, s, 2], tp=core_peer))

        def gathered(k, s):
            near = block_of(k, core_peer, s)
            far = block_of(k, cross_peer, s)
            remote(near, near, tp_send.at[k, s, 0], tp_recv.at[k, s, 0], tp=core_peer).wait_recv()
            remote(far, far, tp_send.at[k, s, 2], tp_recv.at[k, s, 2], tp=core_peer).wait_recv()

        def product(k, w, picked):
            at = pl.ds(0, 2 * rows) if picked is None else pl.ds(picked * rows, rows)
            total = jnp.dot(acts[k, z, at, :], weights[w][...], preferred_element_type=jnp.float32)
            for slot, owner in ((0, my_end), (1, other_hub), (2, other_end)):
                total += jnp.dot(acts[k, owner, at, :], wbuf[w, slot], preferred_element_type=jnp.float32)
            return total

        def stats_out(n, s, summed):
            lane = lax.broadcasted_iota(jnp.int32, (rows, 128), 1)
            sums = jnp.sum(summed, axis=1, keepdims=True)
            squares = jnp.sum(summed * summed, axis=1, keepdims=True)
            table = jnp.where(lane == 0, sums, jnp.where(lane == 1, squares, 0.0))
            stat[n, s, j] = table.T[:8]
            for at, peer in enumerate((chip_peer, cross_peer, core_peer)):
                go(remote(stat.at[n, s, j], stat.at[n, s, j], stat_send.at[n, s, at], stat_recv.at[n, s, at], tp=peer))

        def normed(n, s, summed, gain_vec):
            for at, peer in enumerate((chip_peer, cross_peer, core_peer)):
                remote(stat.at[n, s, peer], stat.at[n, s, peer], stat_send.at[n, s, at], stat_recv.at[n, s, at], tp=peer).wait_recv()
            table = stat[n, s, 0]
            for owner in range(1, n_tp):
                table += stat[n, s, owner]
            columns = jnp.concatenate([table, jnp.zeros((120, rows), jnp.float32)], axis=0).T
            row_mean = columns[:, 0:1] / features
            row_var = columns[:, 1:2] / features - row_mean * row_mean
            return ((summed - row_mean) * lax.rsqrt(row_var + norm_eps) * gain_vec[...]).astype(jnp.bfloat16)

        def put_act(k, s, value):
            acts[k, j, pl.ds(s * rows, rows), :] = value

        def get_act(k, s):
            return acts[k, j, pl.ds(s * rows, rows), :].astype(jnp.float32)

        order = (1, 0)
        own_out(0)
        spread(0, 0, tok)
        own_out(1)
        put_act(0, 0, tok[...])
        tok_copy().wait_recv()
        spread(0, 1)
        end_through(0)
        own_out(2)
        relay(0, 0)
        share(0, 0)
        share(1, 0)
        relay(0, 1)
        end_through(1)
        own_out(3)
        share(0, 1)
        share(2, 0)
        for s in order:
            gathered(0, s)
        complete(0)
        first_act = product(0, 0, None)
        end_through(2)
        own_out(4)
        share(1, 1)
        share(3, 0)
        complete(1)
        second_act = product(0, 1, None)
        hidden = (jax.nn.silu(first_act) * second_act).astype(jnp.bfloat16)
        for s in order:
            put_act(1, s, hidden[s * rows : (s + 1) * rows])
            spread(1, s)
        end_through(3)
        own_out(5)
        share(2, 1)
        for s in order:
            relay(1, s)
        share(4, 0)
        for s in order:
            gathered(1, s)
        complete(2)
        branch = product(1, 2, None)
        sums = [None, None]
        for s in order:
            sums[s] = alpha_scale * get_act(0, s) + 0.5 * branch[s * rows : (s + 1) * rows]
            stats_out(0, s, sums[s])
        end_through(4)
        share(3, 1)
        for s in order:
            put_act(2, s, normed(0, s, sums[s], gain_one))
            spread(2, s)
        share(5, 0)
        for s in order:
            relay(2, s)
        for s in order:
            gathered(2, s)
        complete(3)
        stream = product(2, 3, None).astype(jnp.bfloat16)
        group = j * 4 // n_tp
        window = 2 * (1 + group % 2) * (1 + 3 * (group // 2))
        offset = lax.broadcasted_iota(jnp.int32, (rows, rows), 0) - lax.broadcasted_iota(jnp.int32, (rows, rows), 1)
        band = jnp.where((offset >= 0) & (offset < window), 1.0, 0.0).astype(jnp.bfloat16)
        counts = jnp.minimum(lax.broadcasted_iota(jnp.int32, (rows, 1), 0) + 1, window).astype(jnp.float32)
        pooled = [None, None]
        for s in order:
            piece = stream[s * rows : (s + 1) * rows]
            pooled[s] = jnp.dot(band, piece, preferred_element_type=jnp.float32) / counts - piece.astype(jnp.float32)
        end_through(5)
        share(4, 1)
        share(5, 1)
        complete(4)
        for s in order:
            gate_act = product(2, 4, s)
            put_act(3, s, (pooled[s] * jax.nn.silu(gate_act)).astype(jnp.bfloat16))
            spread(3, s)
        complete(5)
        for s in order:
            relay(3, s)
            gathered(3, s)
            sums[s] = alpha_scale * get_act(2, s) + product(3, 5, s)
            stats_out(1, s, sums[s])
            put_act(4, s, normed(1, s, sums[s], gain_two))
            spread(4, s)
        for s in order:
            relay(4, s)
            gathered(4, s)
            put_act(5, s, (jax.nn.silu(product(4, 0, s)) * product(4, 1, s)).astype(jnp.bfloat16))
            spread(5, s)
        for s in order:
            relay(5, s)
            gathered(5, s)
            sums[s] = alpha_scale * get_act(4, s) + 0.5 * product(5, 2, s)
            stats_out(2, s, sums[s])
            result = normed(2, s, sums[s], gain_three)
            if s == 1:
                landed[...] = result
                go(remote(landed, landed, out_sem.at[0], out_sem.at[1], fs=my_end))
            else:
                out[...] = result
        for copy in started:
            copy.wait_send()


def hub_layer(axis_sizes, tokens, *params):
    batch, rows, width = tokens.shape
    weights, gains = params[:N_WEIGHTS], params[N_WEIGHTS:]
    depth, columns = weights[0].shape
    n_fs, n_tp = axis_sizes
    whole = pl.BlockSpec(memory_space=pltpu.VMEM)
    dma = pltpu.SemaphoreType.DMA
    result = pl.pallas_call(
        functools.partial(hub_kernel, axis_sizes),
        out_shape=jax.ShapeDtypeStruct((rows, width), jnp.bfloat16),
        in_specs=[whole] * (1 + len(params)),
        out_specs=whole,
        scratch_shapes=[
            pltpu.VMEM((N_WEIGHTS, 3, depth, columns), jnp.bfloat16),
            pltpu.VMEM((6, n_tp, 2 * rows, width), jnp.bfloat16),
            pltpu.VMEM((3, 2, n_tp, 8, rows), jnp.float32),
            pltpu.VMEM((rows, width), jnp.bfloat16),
            dma((2,)),
            dma((N_WEIGHTS, 2)),
            dma((N_WEIGHTS, 2)),
            dma((N_WEIGHTS, 2)),
            dma((N_WEIGHTS, 2)),
            dma((N_WEIGHTS, 2)),
            dma((N_WEIGHTS, 2)),
            dma((6, 2, 3)),
            dma((6, 2, 3)),
            dma((3, 2, 3)),
            dma((3, 2, 3)),
            dma((2,)),
        ],
        compiler_params=pltpu.CompilerParams(collective_id=0, has_side_effects=True, vmem_limit_bytes=60 * 2**20),
    )(tokens.reshape(rows, width), *weights, *[gain.reshape(1, -1) for gain in gains])
    return result.reshape(batch, rows, width)


def solution(mesh):
    placed = (
        P(("rep", "fs"), None, "tp"),
        P("fs", "tp"),
        P("fs", "tp"),
        P("fs", "tp"),
        P("fs", "tp"),
        P("fs", "tp"),
        P("fs", "tp"),
        P("tp"),
        P("tp"),
        P("tp"),
    )
    n_rep, n_fs, n_tp = mesh.shape["rep"], mesh.shape["fs"], mesh.shape["tp"]
    hubs = n_rep % 2 == 0 and n_fs == 4 and n_tp == 4
    body = functools.partial(hub_layer, (n_fs, n_tp)) if hubs else shards
    return jax.shard_map(
        body, mesh=mesh, in_specs=placed, out_specs=P(("rep", "fs"), None, "tp"), check_vma=False
    )
```

```python
import functools

import jax
import jax.numpy as jnp
from jax import lax
from jax.experimental import pallas as pl
from jax.experimental.pallas import tpu as pltpu
from jax.sharding import PartitionSpec as P

alpha_scale = 2.0**0.5
norm_eps = 1e-05


def product(inputs, weight):
    return jnp.einsum("bsd,df->bsf", inputs, weight, preferred_element_type=jnp.float32)


def widen(local_rows):
    return lax.all_gather(local_rows, "tp", axis=2, tiled=True)


def norm_cols(summed, gain_vec):
    width = summed.shape[-1] * lax.axis_size("tp")
    totals, squares = lax.psum((jnp.sum(summed, axis=-1), jnp.sum(summed * summed, axis=-1)), "tp")
    row_mean = totals / width
    row_var = squares / width - row_mean * row_mean
    normed = (summed - row_mean[..., None]) * lax.rsqrt(row_var[..., None] + norm_eps)
    return (normed * gain_vec[None, None, :]).astype(jnp.bfloat16)


def half_step(local_rows, project_in, project_out, gain_vec):
    whole = widen(local_rows)
    first_act, second_act = project_in(whole)
    hidden = (jax.nn.silu(first_act) * second_act).astype(jnp.bfloat16)
    wide_hidden = lax.all_gather(hidden, "tp", axis=2, tiled=True)
    branch = project_out(wide_hidden)
    return norm_cols(alpha_scale * local_rows.astype(jnp.float32) + 0.5 * branch, gain_vec)


def pool_mix(local_rows, project_in, project_out, gain_vec):
    whole = widen(local_rows)
    stream_act, gate_act = project_in(whole)
    stream = stream_act.astype(jnp.bfloat16)
    length = stream.shape[1]
    channel_group = lax.axis_index("tp") * 4 // lax.axis_size("tp")
    window = lax.shift_left(jnp.int32(2), channel_group)
    later = lax.broadcasted_iota(jnp.int32, (length, length), 0)
    earlier = lax.broadcasted_iota(jnp.int32, (length, length), 1)
    offset = later - earlier
    band = ((offset >= 0) & (offset < window)).astype(jnp.bfloat16)
    window_sums = jnp.einsum("ts,bsc->btc", band, stream, preferred_element_type=jnp.float32)
    counts = jnp.minimum(jnp.arange(length, dtype=jnp.int32) + 1, window).astype(jnp.float32)
    pooled = window_sums / counts[None, :, None] - stream.astype(jnp.float32)
    gated = (pooled * jax.nn.silu(gate_act)).astype(jnp.bfloat16)
    wide_gated = lax.all_gather(gated, "tp", axis=2, tiled=True)
    branch = project_out(wide_gated)
    return norm_cols(alpha_scale * local_rows.astype(jnp.float32) + branch, gain_vec)


def shards(
    tokens,
    ff_first,
    ff_second,
    ff_down,
    mix_stream,
    mix_gate,
    mix_down,
    gain_one,
    gain_two,
    gain_three,
):
    collected = (
        lax.all_gather(ff_first, "fs", axis=0, tiled=True),
        lax.all_gather(ff_second, "fs", axis=0, tiled=True),
        lax.all_gather(ff_down, "fs", axis=0, tiled=True),
        lax.all_gather(mix_stream, "fs", axis=0, tiled=True),
        lax.all_gather(mix_gate, "fs", axis=0, tiled=True),
        lax.all_gather(mix_down, "fs", axis=0, tiled=True),
    )

    def ffn_in(whole):
        return (product(whole, collected[0]), product(whole, collected[1]))

    def ffn_out(wide_rows):
        return product(wide_rows, collected[2])

    def mix_in(whole):
        return (product(whole, collected[3]), product(whole, collected[4]))

    def mix_out(wide_rows):
        return product(wide_rows, collected[5])

    first = half_step(tokens, ffn_in, ffn_out, gain_one)
    second = pool_mix(first, mix_in, mix_out, gain_two)
    return half_step(second, ffn_in, ffn_out, gain_three)


N_WEIGHTS = 6
MESH = pl.DeviceIdType.MESH


def hub_kernel(
    axis_sizes,
    tok,
    wa,
    wb,
    wc,
    ws,
    wg,
    wm,
    gain_one,
    gain_two,
    gain_three,
    out,
    wbuf,
    acts,
    stat,
    landed,
    tok_sem,
    end_send,
    end_recv,
    mid_send,
    mid_recv,
    rep_send,
    rep_recv,
    tp_send,
    tp_recv,
    stat_send,
    stat_recv,
    out_sem,
):
    n_fs, n_tp = axis_sizes
    weights = (wa, wb, wc, ws, wg, wm)
    rows, width = tok.shape
    depth = wa.shape[0]
    half = depth // 2
    features = width * n_tp
    r = lax.axis_index("rep")
    z = lax.axis_index("fs")
    j = lax.axis_index("tp")
    side = r % 2
    pair = r + 1 - 2 * side
    core_peer = j + 1 - 2 * (j % 2)
    chip_peer = (j + 2) % n_tp
    cross_peer = (core_peer + 2) % n_tp
    upper = z // 2
    is_hub = (z + 1) // 2 == 1
    my_end = upper * (n_fs - 1)
    my_hub = 1 + upper
    other_hub = n_fs - 1 - my_hub
    other_end = n_fs - 1 - my_end

    barrier = pltpu.get_barrier_semaphore()

    def greet(**where):
        pl.semaphore_signal(barrier, inc=1, device_id=where, device_id_type=MESH)

    greet(tp=core_peer)
    greet(tp=chip_peer)
    greet(tp=cross_peer)

    @pl.when(is_hub)
    def _():
        greet(rep=pair)
        greet(fs=other_hub)
        greet(fs=my_end)
        pl.semaphore_wait(barrier, 6)

    @pl.when(jnp.logical_not(is_hub))
    def _():
        greet(fs=my_hub)
        pl.semaphore_wait(barrier, 4)

    def remote(src, dst, send_sem, recv_sem, **where):
        return pltpu.make_async_remote_copy(
            src_ref=src, dst_ref=dst, send_sem=send_sem, recv_sem=recv_sem, device_id=where, device_id_type=MESH
        )

    def part(ref, which):
        return ref.at[pl.ds(pl.multiple_of(which * half, half), half)]

    def seq(ref, s):
        return ref.at[pl.ds(s * rows, rows)]

    def tok_copy():
        return remote(tok, seq(acts.at[0, j], 1), tok_sem.at[0], tok_sem.at[1], fs=my_hub)

    def end_copy(w, order):
        which = side if order == 0 else 1 - side
        return remote(part(weights[w], which), part(wbuf.at[w, 0], which), end_send.at[w, order], end_recv.at[w, order], fs=my_hub)

    @pl.when(jnp.logical_not(is_hub))
    def _():
        started = [tok_copy()] + [end_copy(0, 0)]
        for w in range(1, N_WEIGHTS):
            started += [end_copy(w, 0), end_copy(w - 1, 1)]
        started.append(end_copy(N_WEIGHTS - 1, 1))
        for copy in started:
            copy.start()
        for copy in started:
            copy.wait_send()
        remote(landed, landed, out_sem.at[0], out_sem.at[1], fs=my_hub).wait_recv()
        out[...] = landed[...]

    @pl.when(is_hub)
    def _():
        started = []

        def go(copy):
            copy.start()
            started.append(copy)

        def own_out(w):
            go(remote(part(weights[w], side), part(wbuf.at[w, 1], side), mid_send.at[w, 0], mid_recv.at[w, 0], fs=other_hub))

        def end_through(w):
            end_copy(w, 0).wait_recv()
            go(remote(part(wbuf.at[w, 0], side), part(wbuf.at[w, 2], side), mid_send.at[w, 1], mid_recv.at[w, 1], fs=other_hub))

        def share(w, slot):
            piece = part(wbuf.at[w, 1 + slot], side)
            remote(piece, piece, mid_send.at[w, slot], mid_recv.at[w, slot], fs=other_hub).wait_recv()
            go(remote(piece, piece, rep_send.at[w, slot], rep_recv.at[w, slot], rep=pair))

        def complete(w):
            end_copy(w, 1).wait_recv()
            for slot in range(2):
                piece = part(wbuf.at[w, 1 + slot], 1 - side)
                remote(piece, piece, rep_send.at[w, slot], rep_recv.at[w, slot], rep=pair).wait_recv()

        def block_of(k, owner, s):
            return seq(acts.at[k, owner], s)

        def spread(k, s, src=None):
            mine = block_of(k, j, s)
            src = mine if src is None else src
            go(remote(src, mine, tp_send.at[k, s, 1], tp_recv.at[k, s, 1], tp=chip_peer))
            go(remote(src, mine, tp_send.at[k, s, 0], tp_recv.at[k, s, 0], tp=core_peer))

        def relay(k, s):
            there = block_of(k, chip_peer, s)
            remote(there, there, tp_send.at[k, s, 1], tp_recv.at[k, s, 1], tp=chip_peer).wait_recv()
            go(remote(there, there, tp_send.at[k, s, 2], tp_recv.at[k, s, 2], tp=core_peer))

        def gathered(k, s):
            near = block_of(k, core_peer, s)
            far = block_of(k, cross_peer, s)
            remote(near, near, tp_send.at[k, s, 0], tp_recv.at[k, s, 0], tp=core_peer).wait_recv()
            remote(far, far, tp_send.at[k, s, 2], tp_recv.at[k, s, 2], tp=core_peer).wait_recv()

        def product(k, w, picked):
            at = pl.ds(0, 2 * rows) if picked is None else pl.ds(picked * rows, rows)
            total = jnp.dot(acts[k, z, at, :], weights[w][...], preferred_element_type=jnp.float32)
            for slot, owner in ((0, my_end), (1, other_hub), (2, other_end)):
                total += jnp.dot(acts[k, owner, at, :], wbuf[w, slot], preferred_element_type=jnp.float32)
            return total

        def stats_out(n, s, summed):
            lane = lax.broadcasted_iota(jnp.int32, (rows, 128), 1)
            sums = jnp.sum(summed, axis=1, keepdims=True)
            squares = jnp.sum(summed * summed, axis=1, keepdims=True)
            table = jnp.where(lane == 0, sums, jnp.where(lane == 1, squares, 0.0))
            stat[n, s, j] = table.T[:8]
            for at, peer in enumerate((chip_peer, cross_peer, core_peer)):
                go(remote(stat.at[n, s, j], stat.at[n, s, j], stat_send.at[n, s, at], stat_recv.at[n, s, at], tp=peer))

        def normed(n, s, summed, gain_vec):
            for at, peer in enumerate((chip_peer, cross_peer, core_peer)):
                remote(stat.at[n, s, peer], stat.at[n, s, peer], stat_send.at[n, s, at], stat_recv.at[n, s, at], tp=peer).wait_recv()
            table = stat[n, s, 0]
            for owner in range(1, n_tp):
                table += stat[n, s, owner]
            columns = jnp.concatenate([table, jnp.zeros((120, rows), jnp.float32)], axis=0).T
            row_mean = columns[:, 0:1] / features
            row_var = columns[:, 1:2] / features - row_mean * row_mean
            return ((summed - row_mean) * lax.rsqrt(row_var + norm_eps) * gain_vec[...]).astype(jnp.bfloat16)

        def put_act(k, s, value):
            acts[k, j, pl.ds(s * rows, rows), :] = value

        def get_act(k, s):
            return acts[k, j, pl.ds(s * rows, rows), :].astype(jnp.float32)

        order = (1, 0)
        sums = [None, None]
        pooled = [None, None]
        own_out(0)
        spread(0, 0, tok)
        own_out(1)
        put_act(0, 0, tok[...])
        tok_copy().wait_recv()
        spread(0, 1)
        relay(0, 0)
        end_through(0)
        share(0, 0)
        end_through(1)
        own_out(2)
        share(1, 0)
        relay(0, 1)
        share(0, 1)
        end_through(2)
        own_out(3)
        share(1, 1)
        for s in order:
            gathered(0, s)
        complete(0)
        first_act = product(0, 0, None)
        share(2, 0)
        complete(1)
        second_act = product(0, 1, None)
        hidden = (jax.nn.silu(first_act) * second_act).astype(jnp.bfloat16)
        for s in order:
            put_act(1, s, hidden[s * rows : (s + 1) * rows])
            spread(1, s)
        end_through(3)
        own_out(4)
        share(2, 1)
        relay(1, 1)
        share(3, 0)
        relay(1, 0)
        for s in order:
            gathered(1, s)
        complete(2)
        branch = product(1, 2, None)
        for s in order:
            sums[s] = alpha_scale * get_act(0, s) + 0.5 * branch[s * rows : (s + 1) * rows]
            stats_out(0, s, sums[s])
        end_through(4)
        own_out(5)
        share(3, 1)
        for s in order:
            put_act(2, s, normed(0, s, sums[s], gain_one))
            spread(2, s)
        share(4, 0)
        relay(2, 1)
        relay(2, 0)
        end_through(5)
        share(4, 1)
        for s in order:
            gathered(2, s)
        complete(3)
        stream = product(2, 3, None).astype(jnp.bfloat16)
        group = j * 4 // n_tp
        window = 2 * (1 + group % 2) * (1 + 3 * (group // 2))
        offset = lax.broadcasted_iota(jnp.int32, (rows, rows), 0) - lax.broadcasted_iota(jnp.int32, (rows, rows), 1)
        band = jnp.where((offset >= 0) & (offset < window), 1.0, 0.0).astype(jnp.bfloat16)
        counts = jnp.minimum(lax.broadcasted_iota(jnp.int32, (rows, 1), 0) + 1, window).astype(jnp.float32)
        for s in order:
            piece = stream[s * rows : (s + 1) * rows]
            pooled[s] = jnp.dot(band, piece, preferred_element_type=jnp.float32) / counts - piece.astype(jnp.float32)
        share(5, 0)
        complete(4)
        for s in order:
            gate_act = product(2, 4, s)
            put_act(3, s, (pooled[s] * jax.nn.silu(gate_act)).astype(jnp.bfloat16))
            spread(3, s)
        share(5, 1)
        for s in order:
            relay(3, s)
        complete(5)
        for s in order:
            gathered(3, s)
            sums[s] = alpha_scale * get_act(2, s) + product(3, 5, s)
            stats_out(1, s, sums[s])
        for s in order:
            put_act(4, s, normed(1, s, sums[s], gain_two))
            spread(4, s)
        for s in order:
            relay(4, s)
            gathered(4, s)
            put_act(5, s, (jax.nn.silu(product(4, 0, s)) * product(4, 1, s)).astype(jnp.bfloat16))
            spread(5, s)
        for s in order:
            relay(5, s)
            gathered(5, s)
            sums[s] = alpha_scale * get_act(4, s) + 0.5 * product(5, 2, s)
            stats_out(2, s, sums[s])
        landed[...] = normed(2, 1, sums[1], gain_three)
        go(remote(landed, landed, out_sem.at[0], out_sem.at[1], fs=my_end))
        out[...] = normed(2, 0, sums[0], gain_three)
        for copy in started:
            copy.wait_send()


def hub_layer(axis_sizes, tokens, *params):
    batch, rows, width = tokens.shape
    weights, gains = params[:N_WEIGHTS], params[N_WEIGHTS:]
    depth, columns = weights[0].shape
    n_fs, n_tp = axis_sizes
    whole = pl.BlockSpec(memory_space=pltpu.VMEM)
    dma = pltpu.SemaphoreType.DMA
    result = pl.pallas_call(
        functools.partial(hub_kernel, axis_sizes),
        out_shape=jax.ShapeDtypeStruct((rows, width), jnp.bfloat16),
        in_specs=[whole] * (1 + len(params)),
        out_specs=whole,
        scratch_shapes=[
            pltpu.VMEM((N_WEIGHTS, 3, depth, columns), jnp.bfloat16),
            pltpu.VMEM((6, n_tp, 2 * rows, width), jnp.bfloat16),
            pltpu.VMEM((3, 2, n_tp, 8, rows), jnp.float32),
            pltpu.VMEM((rows, width), jnp.bfloat16),
            dma((2,)),
            dma((N_WEIGHTS, 2)),
            dma((N_WEIGHTS, 2)),
            dma((N_WEIGHTS, 2)),
            dma((N_WEIGHTS, 2)),
            dma((N_WEIGHTS, 2)),
            dma((N_WEIGHTS, 2)),
            dma((6, 2, 3)),
            dma((6, 2, 3)),
            dma((3, 2, 3)),
            dma((3, 2, 3)),
            dma((2,)),
        ],
        compiler_params=pltpu.CompilerParams(collective_id=0, has_side_effects=True, vmem_limit_bytes=60 * 2**20),
    )(tokens.reshape(rows, width), *weights, *[gain.reshape(1, -1) for gain in gains])
    return result.reshape(batch, rows, width)


def solution(mesh):
    placed = (
        P(("rep", "fs"), None, "tp"),
        P("fs", "tp"),
        P("fs", "tp"),
        P("fs", "tp"),
        P("fs", "tp"),
        P("fs", "tp"),
        P("fs", "tp"),
        P("tp"),
        P("tp"),
        P("tp"),
    )
    n_rep, n_fs, n_tp = mesh.shape["rep"], mesh.shape["fs"], mesh.shape["tp"]
    hubs = n_rep % 2 == 0 and n_fs == 4 and n_tp == 4
    body = functools.partial(hub_layer, (n_fs, n_tp)) if hubs else shards
    return jax.shard_map(
        body, mesh=mesh, in_specs=placed, out_specs=P(("rep", "fs"), None, "tp"), check_vma=False
    )
```

```python
import functools

import jax
import jax.numpy as jnp
from jax import lax
from jax.experimental import pallas as pl
from jax.experimental.pallas import tpu as pltpu
from jax.sharding import PartitionSpec as P

alpha_scale = 2.0**0.5
norm_eps = 1e-05


def product(inputs, weight):
    return jnp.einsum("bsd,df->bsf", inputs, weight, preferred_element_type=jnp.float32)


def widen(local_rows):
    return lax.all_gather(local_rows, "tp", axis=2, tiled=True)


def norm_cols(summed, gain_vec):
    width = summed.shape[-1] * lax.axis_size("tp")
    totals, squares = lax.psum((jnp.sum(summed, axis=-1), jnp.sum(summed * summed, axis=-1)), "tp")
    row_mean = totals / width
    row_var = squares / width - row_mean * row_mean
    normed = (summed - row_mean[..., None]) * lax.rsqrt(row_var[..., None] + norm_eps)
    return (normed * gain_vec[None, None, :]).astype(jnp.bfloat16)


def half_step(local_rows, project_in, project_out, gain_vec):
    whole = widen(local_rows)
    first_act, second_act = project_in(whole)
    hidden = (jax.nn.silu(first_act) * second_act).astype(jnp.bfloat16)
    wide_hidden = lax.all_gather(hidden, "tp", axis=2, tiled=True)
    branch = project_out(wide_hidden)
    return norm_cols(alpha_scale * local_rows.astype(jnp.float32) + 0.5 * branch, gain_vec)


def pool_mix(local_rows, project_in, project_out, gain_vec):
    whole = widen(local_rows)
    stream_act, gate_act = project_in(whole)
    stream = stream_act.astype(jnp.bfloat16)
    length = stream.shape[1]
    channel_group = lax.axis_index("tp") * 4 // lax.axis_size("tp")
    window = lax.shift_left(jnp.int32(2), channel_group)
    later = lax.broadcasted_iota(jnp.int32, (length, length), 0)
    earlier = lax.broadcasted_iota(jnp.int32, (length, length), 1)
    offset = later - earlier
    band = ((offset >= 0) & (offset < window)).astype(jnp.bfloat16)
    window_sums = jnp.einsum("ts,bsc->btc", band, stream, preferred_element_type=jnp.float32)
    counts = jnp.minimum(jnp.arange(length, dtype=jnp.int32) + 1, window).astype(jnp.float32)
    pooled = window_sums / counts[None, :, None] - stream.astype(jnp.float32)
    gated = (pooled * jax.nn.silu(gate_act)).astype(jnp.bfloat16)
    wide_gated = lax.all_gather(gated, "tp", axis=2, tiled=True)
    branch = project_out(wide_gated)
    return norm_cols(alpha_scale * local_rows.astype(jnp.float32) + branch, gain_vec)


def shards(
    tokens,
    ff_first,
    ff_second,
    ff_down,
    mix_stream,
    mix_gate,
    mix_down,
    gain_one,
    gain_two,
    gain_three,
):
    collected = (
        lax.all_gather(ff_first, "fs", axis=0, tiled=True),
        lax.all_gather(ff_second, "fs", axis=0, tiled=True),
        lax.all_gather(ff_down, "fs", axis=0, tiled=True),
        lax.all_gather(mix_stream, "fs", axis=0, tiled=True),
        lax.all_gather(mix_gate, "fs", axis=0, tiled=True),
        lax.all_gather(mix_down, "fs", axis=0, tiled=True),
    )

    def ffn_in(whole):
        return (product(whole, collected[0]), product(whole, collected[1]))

    def ffn_out(wide_rows):
        return product(wide_rows, collected[2])

    def mix_in(whole):
        return (product(whole, collected[3]), product(whole, collected[4]))

    def mix_out(wide_rows):
        return product(wide_rows, collected[5])

    first = half_step(tokens, ffn_in, ffn_out, gain_one)
    second = pool_mix(first, mix_in, mix_out, gain_two)
    return half_step(second, ffn_in, ffn_out, gain_three)


N_WEIGHTS = 6
CUTS = 2
MESH = pl.DeviceIdType.MESH


def hub_kernel(
    axis_sizes,
    tok,
    wa,
    wb,
    wc,
    ws,
    wg,
    wm,
    gain_one,
    gain_two,
    gain_three,
    out,
    wbuf,
    acts,
    stat,
    landed,
    tok_sem,
    end_send,
    end_recv,
    mid_send,
    mid_recv,
    rep_send,
    rep_recv,
    tp_send,
    tp_recv,
    stat_send,
    stat_recv,
    out_sem,
):
    n_fs, n_tp = axis_sizes
    weights = (wa, wb, wc, ws, wg, wm)
    rows, width = tok.shape
    depth = wa.shape[0]
    half = depth // (2 * CUTS)
    pieces = N_WEIGHTS * CUTS
    features = width * n_tp
    r = lax.axis_index("rep")
    z = lax.axis_index("fs")
    j = lax.axis_index("tp")
    side = r % 2
    pair = r + 1 - 2 * side
    core_peer = j + 1 - 2 * (j % 2)
    chip_peer = (j + 2) % n_tp
    cross_peer = (core_peer + 2) % n_tp
    upper = z // 2
    is_hub = (z + 1) // 2 == 1
    my_end = upper * (n_fs - 1)
    my_hub = 1 + upper
    other_hub = n_fs - 1 - my_hub
    other_end = n_fs - 1 - my_end

    barrier = pltpu.get_barrier_semaphore()

    def greet(**where):
        pl.semaphore_signal(barrier, inc=1, device_id=where, device_id_type=MESH)

    greet(tp=core_peer)
    greet(tp=chip_peer)
    greet(tp=cross_peer)

    @pl.when(is_hub)
    def _():
        greet(rep=pair)
        greet(fs=other_hub)
        greet(fs=my_end)
        pl.semaphore_wait(barrier, 6)

    @pl.when(jnp.logical_not(is_hub))
    def _():
        greet(fs=my_hub)
        pl.semaphore_wait(barrier, 4)

    def remote(src, dst, send_sem, recv_sem, **where):
        return pltpu.make_async_remote_copy(
            src_ref=src, dst_ref=dst, send_sem=send_sem, recv_sem=recv_sem, device_id=where, device_id_type=MESH
        )

    def part(ref, u, which):
        return ref.at[pl.ds(pl.multiple_of((2 * (u % CUTS) + which) * half, half), half)]

    def seq(ref, s):
        return ref.at[pl.ds(s * rows, rows)]

    def tok_copy():
        return remote(tok, seq(acts.at[0, j], 1), tok_sem.at[0], tok_sem.at[1], fs=my_hub)

    def end_copy(u, order):
        which = side if order == 0 else 1 - side
        return remote(part(weights[u // CUTS], u, which), part(wbuf.at[u // CUTS, 0], u, which), end_send.at[u, order], end_recv.at[u, order], fs=my_hub)

    @pl.when(jnp.logical_not(is_hub))
    def _():
        ahead = 3
        started = [tok_copy()] + [end_copy(u, 0) for u in range(ahead)]
        for u in range(pieces):
            started.append(end_copy(u, 1))
            if u + ahead < pieces:
                started.append(end_copy(u + ahead, 0))
        for copy in started:
            copy.start()
        for copy in started:
            copy.wait_send()
        remote(landed, landed, out_sem.at[0], out_sem.at[1], fs=my_hub).wait_recv()
        out[...] = landed[...]

    @pl.when(is_hub)
    def _():
        started = []

        def go(copy):
            copy.start()
            started.append(copy)

        def own_piece(u):
            w = u // CUTS
            go(remote(part(weights[w], u, side), part(wbuf.at[w, 1], u, side), mid_send.at[u, 0], mid_recv.at[u, 0], fs=other_hub))

        def end_piece(u):
            w = u // CUTS
            end_copy(u, 0).wait_recv()
            go(remote(part(wbuf.at[w, 0], u, side), part(wbuf.at[w, 2], u, side), mid_send.at[u, 1], mid_recv.at[u, 1], fs=other_hub))

        def share_piece(u, slot):
            piece = part(wbuf.at[u // CUTS, 1 + slot], u, side)
            remote(piece, piece, mid_send.at[u, slot], mid_recv.at[u, slot], fs=other_hub).wait_recv()
            go(remote(piece, piece, rep_send.at[u, slot], rep_recv.at[u, slot], rep=pair))

        def of(w):
            return range(CUTS * w, CUTS * w + CUTS)

        def own_out(w):
            for u in of(w):
                own_piece(u)

        def end_through(w):
            for u in of(w):
                end_piece(u)

        def share(w, slot):
            for u in of(w):
                share_piece(u, slot)

        def complete(w):
            for u in of(w):
                end_copy(u, 1).wait_recv()
                for slot in range(2):
                    piece = part(wbuf.at[w, 1 + slot], u, 1 - side)
                    remote(piece, piece, rep_send.at[u, slot], rep_recv.at[u, slot], rep=pair).wait_recv()

        def block_of(k, owner, s):
            return seq(acts.at[k, owner], s)

        def spread(k, s, src=None):
            mine = block_of(k, j, s)
            src = mine if src is None else src
            go(remote(src, mine, tp_send.at[k, s, 1], tp_recv.at[k, s, 1], tp=chip_peer))
            go(remote(src, mine, tp_send.at[k, s, 0], tp_recv.at[k, s, 0], tp=core_peer))

        def relay(k, s):
            there = block_of(k, chip_peer, s)
            remote(there, there, tp_send.at[k, s, 1], tp_recv.at[k, s, 1], tp=chip_peer).wait_recv()
            go(remote(there, there, tp_send.at[k, s, 2], tp_recv.at[k, s, 2], tp=core_peer))

        def gathered(k, s):
            near = block_of(k, core_peer, s)
            far = block_of(k, cross_peer, s)
            remote(near, near, tp_send.at[k, s, 0], tp_recv.at[k, s, 0], tp=core_peer).wait_recv()
            remote(far, far, tp_send.at[k, s, 2], tp_recv.at[k, s, 2], tp=core_peer).wait_recv()

        def product(k, w, picked):
            at = pl.ds(0, 2 * rows) if picked is None else pl.ds(picked * rows, rows)
            total = jnp.dot(acts[k, z, at, :], weights[w][...], preferred_element_type=jnp.float32)
            for slot, owner in ((0, my_end), (1, other_hub), (2, other_end)):
                total += jnp.dot(acts[k, owner, at, :], wbuf[w, slot], preferred_element_type=jnp.float32)
            return total

        def stats_out(n, s, summed):
            lane = lax.broadcasted_iota(jnp.int32, (rows, 128), 1)
            sums = jnp.sum(summed, axis=1, keepdims=True)
            squares = jnp.sum(summed * summed, axis=1, keepdims=True)
            table = jnp.where(lane == 0, sums, jnp.where(lane == 1, squares, 0.0))
            stat[n, s, j] = table.T[:8]
            for at, peer in enumerate((chip_peer, cross_peer, core_peer)):
                go(remote(stat.at[n, s, j], stat.at[n, s, j], stat_send.at[n, s, at], stat_recv.at[n, s, at], tp=peer))

        def normed(n, s, summed, gain_vec):
            for at, peer in enumerate((chip_peer, cross_peer, core_peer)):
                remote(stat.at[n, s, peer], stat.at[n, s, peer], stat_send.at[n, s, at], stat_recv.at[n, s, at], tp=peer).wait_recv()
            table = stat[n, s, 0]
            for owner in range(1, n_tp):
                table += stat[n, s, owner]
            columns = jnp.concatenate([table, jnp.zeros((120, rows), jnp.float32)], axis=0).T
            row_mean = columns[:, 0:1] / features
            row_var = columns[:, 1:2] / features - row_mean * row_mean
            return ((summed - row_mean) * lax.rsqrt(row_var + norm_eps) * gain_vec[...]).astype(jnp.bfloat16)

        def put_act(k, s, value):
            acts[k, j, pl.ds(s * rows, rows), :] = value

        def get_act(k, s):
            return acts[k, j, pl.ds(s * rows, rows), :].astype(jnp.float32)

        order = (1, 0)
        sums = [None, None]
        pooled = [None, None]
        own_out(0)
        spread(0, 0, tok)
        own_out(1)
        put_act(0, 0, tok[...])
        tok_copy().wait_recv()
        spread(0, 1)
        for u in of(0):
            end_piece(u)
            share_piece(u, 0)
        relay(0, 0)
        for u in of(1):
            end_piece(u)
            share_piece(u, 0)
        own_out(2)
        relay(0, 1)
        share(0, 1)
        end_through(2)
        own_out(3)
        share(1, 1)
        for s in order:
            gathered(0, s)
        complete(0)
        first_act = product(0, 0, None)
        share(2, 0)
        complete(1)
        second_act = product(0, 1, None)
        hidden = (jax.nn.silu(first_act) * second_act).astype(jnp.bfloat16)
        for s in order:
            put_act(1, s, hidden[s * rows : (s + 1) * rows])
            spread(1, s)
        end_through(3)
        own_out(4)
        share(2, 1)
        relay(1, 1)
        share(3, 0)
        relay(1, 0)
        for s in order:
            gathered(1, s)
        complete(2)
        branch = product(1, 2, None)
        for s in order:
            sums[s] = alpha_scale * get_act(0, s) + 0.5 * branch[s * rows : (s + 1) * rows]
            stats_out(0, s, sums[s])
        end_through(4)
        own_out(5)
        share(3, 1)
        for s in order:
            put_act(2, s, normed(0, s, sums[s], gain_one))
            spread(2, s)
        share(4, 0)
        relay(2, 1)
        relay(2, 0)
        end_through(5)
        share(4, 1)
        for s in order:
            gathered(2, s)
        complete(3)
        stream = product(2, 3, None).astype(jnp.bfloat16)
        group = j * 4 // n_tp
        window = 2 * (1 + group % 2) * (1 + 3 * (group // 2))
        offset = lax.broadcasted_iota(jnp.int32, (rows, rows), 0) - lax.broadcasted_iota(jnp.int32, (rows, rows), 1)
        band = jnp.where((offset >= 0) & (offset < window), 1.0, 0.0).astype(jnp.bfloat16)
        counts = jnp.minimum(lax.broadcasted_iota(jnp.int32, (rows, 1), 0) + 1, window).astype(jnp.float32)
        for s in order:
            piece = stream[s * rows : (s + 1) * rows]
            pooled[s] = jnp.dot(band, piece, preferred_element_type=jnp.float32) / counts - piece.astype(jnp.float32)
        share(5, 0)
        complete(4)
        for s in order:
            gate_act = product(2, 4, s)
            put_act(3, s, (pooled[s] * jax.nn.silu(gate_act)).astype(jnp.bfloat16))
            spread(3, s)
        share(5, 1)
        for s in order:
            relay(3, s)
        complete(5)
        for s in order:
            gathered(3, s)
            sums[s] = alpha_scale * get_act(2, s) + product(3, 5, s)
            stats_out(1, s, sums[s])
        for s in order:
            put_act(4, s, normed(1, s, sums[s], gain_two))
            spread(4, s)
        for s in order:
            relay(4, s)
            gathered(4, s)
            put_act(5, s, (jax.nn.silu(product(4, 0, s)) * product(4, 1, s)).astype(jnp.bfloat16))
            spread(5, s)
        for s in order:
            relay(5, s)
            gathered(5, s)
            sums[s] = alpha_scale * get_act(4, s) + 0.5 * product(5, 2, s)
            stats_out(2, s, sums[s])
        landed[...] = normed(2, 1, sums[1], gain_three)
        go(remote(landed, landed, out_sem.at[0], out_sem.at[1], fs=my_end))
        out[...] = normed(2, 0, sums[0], gain_three)
        for copy in started:
            copy.wait_send()


def hub_layer(axis_sizes, tokens, *params):
    batch, rows, width = tokens.shape
    weights, gains = params[:N_WEIGHTS], params[N_WEIGHTS:]
    depth, columns = weights[0].shape
    n_fs, n_tp = axis_sizes
    whole = pl.BlockSpec(memory_space=pltpu.VMEM)
    dma = pltpu.SemaphoreType.DMA
    result = pl.pallas_call(
        functools.partial(hub_kernel, axis_sizes),
        out_shape=jax.ShapeDtypeStruct((rows, width), jnp.bfloat16),
        in_specs=[whole] * (1 + len(params)),
        out_specs=whole,
        scratch_shapes=[
            pltpu.VMEM((N_WEIGHTS, 3, depth, columns), jnp.bfloat16),
            pltpu.VMEM((6, n_tp, 2 * rows, width), jnp.bfloat16),
            pltpu.VMEM((3, 2, n_tp, 8, rows), jnp.float32),
            pltpu.VMEM((rows, width), jnp.bfloat16),
            dma((2,)),
            dma((N_WEIGHTS * CUTS, 2)),
            dma((N_WEIGHTS * CUTS, 2)),
            dma((N_WEIGHTS * CUTS, 2)),
            dma((N_WEIGHTS * CUTS, 2)),
            dma((N_WEIGHTS * CUTS, 2)),
            dma((N_WEIGHTS * CUTS, 2)),
            dma((6, 2, 3)),
            dma((6, 2, 3)),
            dma((3, 2, 3)),
            dma((3, 2, 3)),
            dma((2,)),
        ],
        compiler_params=pltpu.CompilerParams(collective_id=0, has_side_effects=True, vmem_limit_bytes=60 * 2**20),
    )(tokens.reshape(rows, width), *weights, *[gain.reshape(1, -1) for gain in gains])
    return result.reshape(batch, rows, width)


def solution(mesh):
    placed = (
        P(("rep", "fs"), None, "tp"),
        P("fs", "tp"),
        P("fs", "tp"),
        P("fs", "tp"),
        P("fs", "tp"),
        P("fs", "tp"),
        P("fs", "tp"),
        P("tp"),
        P("tp"),
        P("tp"),
    )
    n_rep, n_fs, n_tp = mesh.shape["rep"], mesh.shape["fs"], mesh.shape["tp"]
    hubs = n_rep % 2 == 0 and n_fs == 4 and n_tp == 4
    body = functools.partial(hub_layer, (n_fs, n_tp)) if hubs else shards
    return jax.shard_map(
        body, mesh=mesh, in_specs=placed, out_specs=P(("rep", "fs"), None, "tp"), check_vma=False
    )
```

```python
import functools

import jax
import jax.numpy as jnp
from jax import lax
from jax.experimental import pallas as pl
from jax.experimental.pallas import tpu as pltpu
from jax.sharding import PartitionSpec as P

alpha_scale = 2.0**0.5
norm_eps = 1e-05


def product(inputs, weight):
    return jnp.einsum("bsd,df->bsf", inputs, weight, preferred_element_type=jnp.float32)


def widen(local_rows):
    return lax.all_gather(local_rows, "tp", axis=2, tiled=True)


def norm_cols(summed, gain_vec):
    width = summed.shape[-1] * lax.axis_size("tp")
    totals, squares = lax.psum((jnp.sum(summed, axis=-1), jnp.sum(summed * summed, axis=-1)), "tp")
    row_mean = totals / width
    row_var = squares / width - row_mean * row_mean
    normed = (summed - row_mean[..., None]) * lax.rsqrt(row_var[..., None] + norm_eps)
    return (normed * gain_vec[None, None, :]).astype(jnp.bfloat16)


def half_step(local_rows, project_in, project_out, gain_vec):
    whole = widen(local_rows)
    first_act, second_act = project_in(whole)
    hidden = (jax.nn.silu(first_act) * second_act).astype(jnp.bfloat16)
    wide_hidden = lax.all_gather(hidden, "tp", axis=2, tiled=True)
    branch = project_out(wide_hidden)
    return norm_cols(alpha_scale * local_rows.astype(jnp.float32) + 0.5 * branch, gain_vec)


def pool_mix(local_rows, project_in, project_out, gain_vec):
    whole = widen(local_rows)
    stream_act, gate_act = project_in(whole)
    stream = stream_act.astype(jnp.bfloat16)
    length = stream.shape[1]
    channel_group = lax.axis_index("tp") * 4 // lax.axis_size("tp")
    window = lax.shift_left(jnp.int32(2), channel_group)
    later = lax.broadcasted_iota(jnp.int32, (length, length), 0)
    earlier = lax.broadcasted_iota(jnp.int32, (length, length), 1)
    offset = later - earlier
    band = ((offset >= 0) & (offset < window)).astype(jnp.bfloat16)
    window_sums = jnp.einsum("ts,bsc->btc", band, stream, preferred_element_type=jnp.float32)
    counts = jnp.minimum(jnp.arange(length, dtype=jnp.int32) + 1, window).astype(jnp.float32)
    pooled = window_sums / counts[None, :, None] - stream.astype(jnp.float32)
    gated = (pooled * jax.nn.silu(gate_act)).astype(jnp.bfloat16)
    wide_gated = lax.all_gather(gated, "tp", axis=2, tiled=True)
    branch = project_out(wide_gated)
    return norm_cols(alpha_scale * local_rows.astype(jnp.float32) + branch, gain_vec)


def shards(
    tokens,
    ff_first,
    ff_second,
    ff_down,
    mix_stream,
    mix_gate,
    mix_down,
    gain_one,
    gain_two,
    gain_three,
):
    collected = (
        lax.all_gather(ff_first, "fs", axis=0, tiled=True),
        lax.all_gather(ff_second, "fs", axis=0, tiled=True),
        lax.all_gather(ff_down, "fs", axis=0, tiled=True),
        lax.all_gather(mix_stream, "fs", axis=0, tiled=True),
        lax.all_gather(mix_gate, "fs", axis=0, tiled=True),
        lax.all_gather(mix_down, "fs", axis=0, tiled=True),
    )

    def ffn_in(whole):
        return (product(whole, collected[0]), product(whole, collected[1]))

    def ffn_out(wide_rows):
        return product(wide_rows, collected[2])

    def mix_in(whole):
        return (product(whole, collected[3]), product(whole, collected[4]))

    def mix_out(wide_rows):
        return product(wide_rows, collected[5])

    first = half_step(tokens, ffn_in, ffn_out, gain_one)
    second = pool_mix(first, mix_in, mix_out, gain_two)
    return half_step(second, ffn_in, ffn_out, gain_three)


N_WEIGHTS = 6
MESH = pl.DeviceIdType.MESH


def hub_kernel(
    axis_sizes,
    tok,
    wa,
    wb,
    wc,
    ws,
    wg,
    wm,
    gain_one,
    gain_two,
    gain_three,
    out,
    wbuf,
    acts,
    stat,
    landed,
    tok_sem,
    end_send,
    end_recv,
    mid_send,
    mid_recv,
    rep_send,
    rep_recv,
    tp_send,
    tp_recv,
    stat_send,
    stat_recv,
    out_sem,
):
    n_fs, n_tp = axis_sizes
    weights = (wa, wb, wc, ws, wg, wm)
    rows, width = tok.shape
    depth = wa.shape[0]
    half = depth // 2
    features = width * n_tp
    r = lax.axis_index("rep")
    z = lax.axis_index("fs")
    j = lax.axis_index("tp")
    side = r % 2
    pair = r + 1 - 2 * side
    core_peer = j + 1 - 2 * (j % 2)
    chip_peer = (j + 2) % n_tp
    cross_peer = (core_peer + 2) % n_tp
    upper = z // 2
    is_hub = (z + 1) // 2 == 1
    my_end = upper * (n_fs - 1)
    my_hub = 1 + upper
    other_hub = n_fs - 1 - my_hub
    other_end = n_fs - 1 - my_end

    barrier = pltpu.get_barrier_semaphore()

    def greet(**where):
        pl.semaphore_signal(barrier, inc=1, device_id=where, device_id_type=MESH)

    greet(tp=core_peer)
    greet(tp=chip_peer)
    greet(tp=cross_peer)

    @pl.when(is_hub)
    def _():
        greet(rep=pair)
        greet(fs=other_hub)
        greet(fs=my_end)
        pl.semaphore_wait(barrier, 6)

    @pl.when(jnp.logical_not(is_hub))
    def _():
        greet(fs=my_hub)
        pl.semaphore_wait(barrier, 4)

    def remote(src, dst, send_sem, recv_sem, **where):
        return pltpu.make_async_remote_copy(
            src_ref=src, dst_ref=dst, send_sem=send_sem, recv_sem=recv_sem, device_id=where, device_id_type=MESH
        )

    def part(ref, which):
        return ref.at[pl.ds(pl.multiple_of(which * half, half), half)]

    def seq(ref, s):
        return ref.at[pl.ds(s * rows, rows)]

    def tok_copy():
        return remote(tok, seq(acts.at[0, j], 1), tok_sem.at[0], tok_sem.at[1], fs=my_hub)

    def end_copy(w, order):
        which = side if order == 0 else 1 - side
        return remote(part(weights[w], which), part(wbuf.at[w, 0], which), end_send.at[w, order], end_recv.at[w, order], fs=my_hub)

    @pl.when(jnp.logical_not(is_hub))
    def _():
        started = [tok_copy()] + [end_copy(0, 0)]
        for w in range(1, N_WEIGHTS):
            started += [end_copy(w, 0), end_copy(w - 1, 1)]
        started.append(end_copy(N_WEIGHTS - 1, 1))
        for copy in started:
            copy.start()
        for copy in started:
            copy.wait_send()
        remote(landed, landed, out_sem.at[0], out_sem.at[1], fs=my_hub).wait_recv()
        out[...] = landed[...]

    @pl.when(is_hub)
    def _():
        started = []

        def go(copy):
            copy.start()
            started.append(copy)

        def own_out(w):
            go(remote(part(weights[w], side), part(wbuf.at[w, 1], side), mid_send.at[w, 0], mid_recv.at[w, 0], fs=other_hub))

        def end_through(w):
            end_copy(w, 0).wait_recv()
            go(remote(part(wbuf.at[w, 0], side), part(wbuf.at[w, 2], side), mid_send.at[w, 1], mid_recv.at[w, 1], fs=other_hub))

        def share(w, slot):
            piece = part(wbuf.at[w, 1 + slot], side)
            remote(piece, piece, mid_send.at[w, slot], mid_recv.at[w, slot], fs=other_hub).wait_recv()
            go(remote(piece, piece, rep_send.at[w, slot], rep_recv.at[w, slot], rep=pair))

        def shared(w, slot):
            piece = part(wbuf.at[w, 1 + slot], 1 - side)
            remote(piece, piece, rep_send.at[w, slot], rep_recv.at[w, slot], rep=pair).wait_recv()

        def mostly(w):
            end_copy(w, 1).wait_recv()
            shared(w, 0)

        def complete(w):
            mostly(w)
            shared(w, 1)

        def block_of(k, owner, s):
            return seq(acts.at[k, owner], s)

        def spread(k, s, src=None):
            mine = block_of(k, j, s)
            src = mine if src is None else src
            go(remote(src, mine, tp_send.at[k, s, 1], tp_recv.at[k, s, 1], tp=chip_peer))
            go(remote(src, mine, tp_send.at[k, s, 0], tp_recv.at[k, s, 0], tp=core_peer))

        def relay(k, s):
            there = block_of(k, chip_peer, s)
            remote(there, there, tp_send.at[k, s, 1], tp_recv.at[k, s, 1], tp=chip_peer).wait_recv()
            go(remote(there, there, tp_send.at[k, s, 2], tp_recv.at[k, s, 2], tp=core_peer))

        def gathered(k, s):
            near = block_of(k, core_peer, s)
            far = block_of(k, cross_peer, s)
            remote(near, near, tp_send.at[k, s, 0], tp_recv.at[k, s, 0], tp=core_peer).wait_recv()
            remote(far, far, tp_send.at[k, s, 2], tp_recv.at[k, s, 2], tp=core_peer).wait_recv()

        def early(k, w, picked):
            at = pl.ds(0, 2 * rows) if picked is None else pl.ds(picked * rows, rows)
            total = jnp.dot(acts[k, z, at, :], weights[w][...], preferred_element_type=jnp.float32)
            for slot, owner in ((0, my_end), (1, other_hub)):
                total += jnp.dot(acts[k, owner, at, :], wbuf[w, slot], preferred_element_type=jnp.float32)
            return total

        def late(k, w, picked):
            at = pl.ds(0, 2 * rows) if picked is None else pl.ds(picked * rows, rows)
            return jnp.dot(acts[k, other_end, at, :], wbuf[w, 2], preferred_element_type=jnp.float32)

        def product(k, w, picked):
            return early(k, w, picked) + late(k, w, picked)

        def stats_out(n, s, summed):
            lane = lax.broadcasted_iota(jnp.int32, (rows, 128), 1)
            sums = jnp.sum(summed, axis=1, keepdims=True)
            squares = jnp.sum(summed * summed, axis=1, keepdims=True)
            table = jnp.where(lane == 0, sums, jnp.where(lane == 1, squares, 0.0))
            stat[n, s, j] = table.T[:8]
            for at, peer in enumerate((chip_peer, cross_peer, core_peer)):
                go(remote(stat.at[n, s, j], stat.at[n, s, j], stat_send.at[n, s, at], stat_recv.at[n, s, at], tp=peer))

        def normed(n, s, summed, gain_vec):
            for at, peer in enumerate((chip_peer, cross_peer, core_peer)):
                remote(stat.at[n, s, peer], stat.at[n, s, peer], stat_send.at[n, s, at], stat_recv.at[n, s, at], tp=peer).wait_recv()
            table = stat[n, s, 0]
            for owner in range(1, n_tp):
                table += stat[n, s, owner]
            columns = jnp.concatenate([table, jnp.zeros((120, rows), jnp.float32)], axis=0).T
            row_mean = columns[:, 0:1] / features
            row_var = columns[:, 1:2] / features - row_mean * row_mean
            return ((summed - row_mean) * lax.rsqrt(row_var + norm_eps) * gain_vec[...]).astype(jnp.bfloat16)

        def put_act(k, s, value):
            acts[k, j, pl.ds(s * rows, rows), :] = value

        def get_act(k, s):
            return acts[k, j, pl.ds(s * rows, rows), :].astype(jnp.float32)

        order = (1, 0)
        sums = [None, None]
        pooled = [None, None]
        own_out(0)
        spread(0, 0, tok)
        own_out(1)
        put_act(0, 0, tok[...])
        tok_copy().wait_recv()
        spread(0, 1)
        relay(0, 0)
        end_through(0)
        share(0, 0)
        end_through(1)
        own_out(2)
        share(1, 0)
        relay(0, 1)
        share(0, 1)
        end_through(2)
        own_out(3)
        share(1, 1)
        for s in order:
            gathered(0, s)
        complete(0)
        first_act = product(0, 0, None)
        share(2, 0)
        complete(1)
        second_act = product(0, 1, None)
        hidden = (jax.nn.silu(first_act) * second_act).astype(jnp.bfloat16)
        for s in order:
            put_act(1, s, hidden[s * rows : (s + 1) * rows])
            spread(1, s)
        end_through(3)
        own_out(4)
        share(2, 1)
        relay(1, 1)
        share(3, 0)
        relay(1, 0)
        for s in order:
            gathered(1, s)
        complete(2)
        branch = product(1, 2, None)
        for s in order:
            sums[s] = alpha_scale * get_act(0, s) + 0.5 * branch[s * rows : (s + 1) * rows]
            stats_out(0, s, sums[s])
        end_through(4)
        own_out(5)
        share(3, 1)
        for s in order:
            put_act(2, s, normed(0, s, sums[s], gain_one))
            spread(2, s)
        share(4, 0)
        relay(2, 1)
        relay(2, 0)
        end_through(5)
        share(4, 1)
        for s in order:
            gathered(2, s)
        complete(3)
        stream = product(2, 3, None).astype(jnp.bfloat16)
        group = j * 4 // n_tp
        window = 2 * (1 + group % 2) * (1 + 3 * (group // 2))
        offset = lax.broadcasted_iota(jnp.int32, (rows, rows), 0) - lax.broadcasted_iota(jnp.int32, (rows, rows), 1)
        band = jnp.where((offset >= 0) & (offset < window), 1.0, 0.0).astype(jnp.bfloat16)
        counts = jnp.minimum(lax.broadcasted_iota(jnp.int32, (rows, 1), 0) + 1, window).astype(jnp.float32)
        for s in order:
            piece = stream[s * rows : (s + 1) * rows]
            pooled[s] = jnp.dot(band, piece, preferred_element_type=jnp.float32) / counts - piece.astype(jnp.float32)
        share(5, 0)
        mostly(4)
        gate_early = early(2, 4, None)
        shared(4, 1)
        for s in order:
            gate_act = gate_early[s * rows : (s + 1) * rows] + late(2, 4, s)
            put_act(3, s, (pooled[s] * jax.nn.silu(gate_act)).astype(jnp.bfloat16))
            spread(3, s)
        share(5, 1)
        relay(3, 1)
        mostly(5)
        for s in order:
            gathered(3, s)
            sums[s] = alpha_scale * get_act(2, s) + early(3, 5, s)
            if s == order[0]:
                relay(3, 0)
                shared(5, 1)
            sums[s] += late(3, 5, s)
            stats_out(1, s, sums[s])
        for s in order:
            put_act(4, s, normed(1, s, sums[s], gain_two))
            spread(4, s)
        for s in order:
            relay(4, s)
            gathered(4, s)
            put_act(5, s, (jax.nn.silu(product(4, 0, s)) * product(4, 1, s)).astype(jnp.bfloat16))
            spread(5, s)
        for s in order:
            relay(5, s)
            gathered(5, s)
            sums[s] = alpha_scale * get_act(4, s) + 0.5 * product(5, 2, s)
            stats_out(2, s, sums[s])
        landed[...] = normed(2, 1, sums[1], gain_three)
        go(remote(landed, landed, out_sem.at[0], out_sem.at[1], fs=my_end))
        out[...] = normed(2, 0, sums[0], gain_three)
        for copy in started:
            copy.wait_send()


def hub_layer(axis_sizes, tokens, *params):
    batch, rows, width = tokens.shape
    weights, gains = params[:N_WEIGHTS], params[N_WEIGHTS:]
    depth, columns = weights[0].shape
    n_fs, n_tp = axis_sizes
    whole = pl.BlockSpec(memory_space=pltpu.VMEM)
    dma = pltpu.SemaphoreType.DMA
    result = pl.pallas_call(
        functools.partial(hub_kernel, axis_sizes),
        out_shape=jax.ShapeDtypeStruct((rows, width), jnp.bfloat16),
        in_specs=[whole] * (1 + len(params)),
        out_specs=whole,
        scratch_shapes=[
            pltpu.VMEM((N_WEIGHTS, 3, depth, columns), jnp.bfloat16),
            pltpu.VMEM((6, n_tp, 2 * rows, width), jnp.bfloat16),
            pltpu.VMEM((3, 2, n_tp, 8, rows), jnp.float32),
            pltpu.VMEM((rows, width), jnp.bfloat16),
            dma((2,)),
            dma((N_WEIGHTS, 2)),
            dma((N_WEIGHTS, 2)),
            dma((N_WEIGHTS, 2)),
            dma((N_WEIGHTS, 2)),
            dma((N_WEIGHTS, 2)),
            dma((N_WEIGHTS, 2)),
            dma((6, 2, 3)),
            dma((6, 2, 3)),
            dma((3, 2, 3)),
            dma((3, 2, 3)),
            dma((2,)),
        ],
        compiler_params=pltpu.CompilerParams(collective_id=0, has_side_effects=True, vmem_limit_bytes=60 * 2**20),
    )(tokens.reshape(rows, width), *weights, *[gain.reshape(1, -1) for gain in gains])
    return result.reshape(batch, rows, width)


def solution(mesh):
    placed = (
        P(("rep", "fs"), None, "tp"),
        P("fs", "tp"),
        P("fs", "tp"),
        P("fs", "tp"),
        P("fs", "tp"),
        P("fs", "tp"),
        P("fs", "tp"),
        P("tp"),
        P("tp"),
        P("tp"),
    )
    n_rep, n_fs, n_tp = mesh.shape["rep"], mesh.shape["fs"], mesh.shape["tp"]
    hubs = n_rep % 2 == 0 and n_fs == 4 and n_tp == 4
    body = functools.partial(hub_layer, (n_fs, n_tp)) if hubs else shards
    return jax.shard_map(
        body, mesh=mesh, in_specs=placed, out_specs=P(("rep", "fs"), None, "tp"), check_vma=False
    )
```
